256 devices in a mesh: kv: 32 (over z, y), tp: 8 (over x, core).
Axes of the slice: x: 4, y: 4, z: 8, core: 2. Of those that a mesh axis runs over, the one named last changes fastest.
Arguments:
- tokens: bfloat16 [64, 4096], P(None, ('kv', 'tp')), may hold values from -8 to 8
- gate_weights: bfloat16 [2, 4096, 11264], P(None, None, ('kv', 'tp')), may hold values from -0.09375 to 0.09375
- up_weights: bfloat16 [2, 4096, 11264], P(None, None, ('kv', 'tp')), may hold values from -0.09375 to 0.09375
- down_weights: bfloat16 [2, 11264, 4096], P(None, ('kv', 'tp')), may hold values from -1 to 1
- norm_gain: bfloat16 [3, 4096], P(None, ('kv', 'tp')), may hold values from 0.25 to 4.5
- norm_bias: bfloat16 [3, 4096], P(None, ('kv', 'tp')), may hold values from -3 to 3
- query_weight: bfloat16 [4096, 4096], P('kv', 'tp'), may hold values from -0.09375 to 0.09375
- forget_weight: bfloat16 [4096, 4096], P('kv', 'tp'), may hold values from -0.09375 to 0.09375
- input_weight: bfloat16 [4096, 4096], P('kv', 'tp'), may hold values from -0.09375 to 0.09375
- outgate_weight: bfloat16 [4096, 4096], P('kv', 'tp'), may hold values from -0.09375 to 0.09375
- lower_bound: float32 [4096], P('tp'), may hold values from 0.05 to 0.9
- head_gain: float32 [4096], P('tp'), may hold values from 0.1 to 1.9
- out_weight: bfloat16 [4096, 4096], P('tp'), may hold values from -0.25 to 0.25
- state: float32 [64, 32, 128, 128], P('kv', 'tp'), may hold values from -3 to 3
Outputs:
- mixed: bfloat16 [64, 4096], P(None, ('kv', 'tp'))
- new_state: float32 [64, 32, 128, 128], P('kv', 'tp')
The draws below stay inside these ranges and needn't reach their ends.
All inputs are finite; a program needn't handle non-finite values.
Results may differ from the reference program's by a relative error of at most 0.022.
Values may be sent and summed in bfloat16 or wider, within the bound.
A program may use at most 64 MiB of HBM per device.

```python
import math
import jax
import jax.numpy as jnp
from jax import lax

D = 4096
FF = 11264
HEAD = 128
HEADS = 32
BATCH = 64


def draw_tokens(key, part):
    position = jnp.arange(D, dtype=jnp.float32)[None, :] / D
    values = jax.random.normal(key, (BATCH, D), jnp.float32) * 0.4 * 4.0 ** position
    return jnp.clip(values, -8.0, 8.0).astype(jnp.bfloat16)


def draw_norm_gain(key, part):
    position = jnp.arange(D, dtype=jnp.float32)[None, :] / D
    jitter = 1.0 + 0.3 * jax.random.uniform(key, (3, D), jnp.float32, -1.0, 1.0)
    values = 0.6 * 3.0 ** position * jitter
    return values.astype(jnp.bfloat16)


def with_spikes(result, own_key, source, target, parts, factor):
    owner, partner = [(jnp.arange(result.shape[dim]) // (result.shape[dim] // parts)).reshape([-1 if axis == dim else 1 for axis in range(result.ndim)]) for dim in (source, target)]
    chosen = jax.random.permutation(own_key, parts)[partner]
    strong = (owner == chosen) | (owner == (partner + parts // 2) % parts)
    return jnp.where(strong, factor * result, result)


def block_scale(key, dims, cuts, least, top_value):
    factor_of, own = 1.0, jax.random.fold_in(key, 6)
    for dim, blocks in cuts:
        steps = jnp.exp(jax.random.uniform(jax.random.fold_in(own, dim), (blocks,), jnp.float32, least / len(cuts), top_value / len(cuts)))
        factor_of = factor_of * jnp.repeat(steps, dims[dim] // blocks).reshape([-1 if axis == dim else 1 for axis in range(len(dims))])
    return factor_of


def noise(rng, shape, scale, bound, cuts=(), held_as=jnp.bfloat16):
    drawn = scale * jax.random.normal(rng, shape, jnp.float32)
    if cuts:
        drawn = drawn * block_scale(rng, shape, cuts, -0.22, 0.18)
    return jnp.clip(drawn, -bound, bound).astype(held_as)


def noise_with(rng, shape, scale, reach, cuts, heavy, held_as=jnp.bfloat16):
    array = scale * jax.random.normal(rng, shape, jnp.float32)
    if cuts:
        array = array * block_scale(rng, shape, cuts, -0.22, 0.18)
    return jnp.clip(with_spikes(array, jax.random.fold_in(rng, 3), *heavy), -reach, reach).astype(held_as)


def setup_inputs(seed: int = 0) -> dict:
    arg_keys = jax.random.split(jax.random.key(seed), 15)
    tokens = draw_tokens(jax.random.fold_in(arg_keys[14], 71), 0)
    gate_weights = noise(arg_keys[1], (2, D, FF), D ** -0.5, 0.09375, ((2, 256),))
    up_weights = noise(arg_keys[2], (2, D, FF), D ** -0.5, 0.09375, ((2, 256),))
    down_weights = noise_with(arg_keys[3], (2, FF, D), (FF // 16) ** -0.5, 1.0, ((1, 256),), (1, 2, 256, 6.0))
    norm_gain = draw_norm_gain(jax.random.fold_in(arg_keys[14], 71), 0)
    norm_bias = noise(arg_keys[5], (3, D), 0.5, 3.0, ((1, 256),))
    query_weight = noise(arg_keys[6], (D, D), D ** -0.5, 0.09375, ((0, 32), (1, 8)))
    forget_weight = noise(arg_keys[7], (D, D), D ** -0.5, 0.09375, ((0, 32), (1, 8)))
    input_weight = noise(arg_keys[8], (D, D), D ** -0.5, 0.09375, ((0, 32), (1, 8)))
    outgate_weight = noise(arg_keys[9], (D, D), D ** -0.5, 0.09375, ((0, 32), (1, 8)))
    lower_bound = jnp.clip(jnp.exp(math.log(0.9) - 2.8903717 * jax.random.uniform(arg_keys[10], (D,), jnp.float32) ** block_scale(arg_keys[10], (D,), ((0, 8),), -0.2, 0.2)), 0.05, 0.9)
    head_gain = jnp.clip(1.0 + 0.18 * jax.random.normal(arg_keys[11], (D,), jnp.float32), 0.1, 1.9)
    out_weight = noise_with(arg_keys[12], (D, D), (D // 4) ** -0.5, 0.25, ((0, 8),), (0, 1, 8, 2.0))
    state = noise(arg_keys[13], (BATCH, HEADS, HEAD, HEAD), 0.5, 3.0, ((0, 32), (1, 8)), jnp.float32)
    return {"tokens": tokens, "gate_weights": gate_weights, "up_weights": up_weights, "down_weights": down_weights, "norm_gain": norm_gain, "norm_bias": norm_bias, "query_weight": query_weight, "forget_weight": forget_weight, "input_weight": input_weight, "outgate_weight": outgate_weight, "lower_bound": lower_bound, "head_gain": head_gain, "out_weight": out_weight, "state": state}


residual_scale = 8.0 ** 0.25
norm_eps = 1e-05
head_eps = 1e-06

def layer_norm(stream, gain_row, bias_row):
    row_mean = lax.optimization_barrier(jnp.mean(stream, axis=-1, keepdims=True))
    centred = stream - row_mean
    spread = lax.optimization_barrier(jnp.mean(centred * centred, axis=-1, keepdims=True))
    return centred * lax.rsqrt(spread + norm_eps) * gain_row.astype(jnp.float32) + bias_row.astype(jnp.float32)

def half_ffn(row_block, gate_w, up_w, down_w):
    gate_proj = jnp.dot(row_block, gate_w, preferred_element_type=jnp.float32)
    up_proj = jnp.dot(row_block, up_w, preferred_element_type=jnp.float32)
    hidden = (jax.nn.silu(gate_proj) * up_proj).astype(jnp.bfloat16)
    return jnp.dot(hidden, down_w, preferred_element_type=jnp.float32)

def reference(tokens, gate_weights, up_weights, down_weights, norm_gain, norm_bias, query_weight, forget_weight, input_weight, outgate_weight, lower_bound, head_gain, out_weight, state):
    head_count = D // HEAD
    row_count = tokens.shape[0]
    branch_one = half_ffn(tokens, gate_weights[0], up_weights[0], down_weights[0])
    stream = residual_scale * tokens.astype(jnp.float32) + 0.5 * branch_one
    normed = layer_norm(stream, norm_gain[0], norm_bias[0]).astype(jnp.bfloat16)
    projected = [jnp.dot(normed, weight, preferred_element_type=jnp.float32).astype(jnp.bfloat16) for weight in (query_weight, forget_weight, input_weight, outgate_weight)]
    shaped = [piece_pre.astype(jnp.float32).reshape(row_count, head_count, HEAD) for piece_pre in projected[:3]]
    low_bound = lower_bound.reshape(head_count, HEAD)

    def one_sequence(pieces):
        query_pre, forget_pre, input_pre, old_state = pieces
        forget = low_bound + (1.0 - low_bound) * jax.nn.sigmoid(forget_pre)
        key_part = (1.0 - low_bound) * jax.nn.sigmoid(-forget_pre)
        updated = forget[:, :, None] * old_state + key_part[:, :, None] * input_pre[:, None, :]
        readout = jnp.einsum('hd,hde->he', jax.nn.silu(query_pre), updated, precision=lax.Precision.HIGHEST)
        return (readout, updated)
    readout, new_state = lax.map(one_sequence, (shaped[0], shaped[1], shaped[2], state))
    readout = readout * lax.rsqrt(lax.optimization_barrier(jnp.mean(readout * readout, axis=-1, keepdims=True)) + head_eps)
    gated_out = (readout.reshape(row_count, D) * head_gain * jax.nn.silu(projected[3].astype(jnp.float32))).astype(jnp.bfloat16)
    mixed_out = jnp.dot(gated_out, out_weight, preferred_element_type=jnp.float32)
    stream = (residual_scale * normed.astype(jnp.float32) + mixed_out).astype(jnp.bfloat16)
    normed = layer_norm(stream.astype(jnp.float32), norm_gain[1], norm_bias[1]).astype(jnp.bfloat16)
    branch_two = half_ffn(normed, gate_weights[1], up_weights[1], down_weights[1])
    stream = residual_scale * normed.astype(jnp.float32) + 0.5 * branch_two
    mixed = layer_norm(stream, norm_gain[2], norm_bias[2]).astype(jnp.bfloat16)
    return (mixed, new_state)
```

```python
import jax
import jax.numpy as jnp
from jax import lax
from jax.experimental import pallas as pl
from jax.experimental.pallas import tpu as pltpu
from jax.sharding import PartitionSpec as P

MESH = pl.DeviceIdType.MESH
BF = jnp.bfloat16
F32 = jnp.float32
NZ, NY, NX, NC = 8, 4, 4, 2
NT = NX * NC
D = 4096
HEAD = 128
NLT = D // 128
RES = 8.0**0.25
NORM_EPS = 1e-05
HEAD_EPS = 1e-06
ORDER8 = (4, 3, 5, 2, 6, 1, 7)
ORDER4 = (2, 1, 3)
NREMOTE = 256
NLOCAL = 120


def nt_dot(a, b):
    return lax.dot_general(a, b, (((1,), (1,)), ((), ())), preferred_element_type=F32)


def nn_dot(a, b):
    return jnp.dot(a, b, preferred_element_type=F32)


def iota(shape, dim):
    return lax.broadcasted_iota(jnp.int32, shape, dim)


def onehot(mask):
    return jnp.where(mask, 1.0, 0.0).astype(BF)


def f32(v):
    return v.astype(F32)


def kernel(
    tok_h, gate_h, up_h, down_h, gain_h, bias_h, wq_h, wf_h, wi_h, wo_h, lb_h, hg_h, outw_h, state_h,
    mixed_ref, ns_h,
    tok_v, gain_v, bias_v, lb_v, hg_v, gate_r, up_r, down_r, w2g, w2u, d2, w4, outw_v, st_v, ns_v,
    g8, ts, tr, xg, gt, gws, gwr, gws2, gwr2, gwt,
    s0, r0, t0, r1, u0, v0, r2, w0, q0, r3, zb,
    se, st, rz, re, rst, sz, szs, rzs, rze, rzst, rz2,
    sf, rf, yz, yg, xn,
    s1, r0b, t1, r1b, u1, v1, r2b, w1, q1, r3b, sa, ra, sb, rb, sv, rv,
    ssem, rsem, lsem,
):
    kv = lax.axis_index("kv")
    tp = lax.axis_index("tp")
    z, y = lax.div(kv, NY), lax.rem(kv, NY)
    x, c = lax.div(tp, NC), lax.rem(tp, NC)

    def dev(z_=None, y_=None, x_=None, c_=None):
        z_, y_ = z if z_ is None else z_, y if y_ is None else y_
        x_, c_ = x if x_ is None else x_, c if c_ is None else c_
        return (z_ * NY + y_, x_ * NC + c_)

    def zz(d):
        return lax.rem(z + d, NZ)

    def yy(d):
        return lax.rem(y + d, NY)

    def xx(d):
        return lax.rem(x + d, NX)

    oc = 1 - c
    tpeers = [(dx, dc) for dc in (1, 0) for dx in (2, 1, 3, 0) if (dx, dc) != (0, 0)]

    sends = []
    count = [0]

    def slot(n=1):
        first = count[0]
        count[0] += n
        assert count[0] <= NREMOTE
        return first

    def rcopy(i, src, dst, device):
        return pltpu.make_async_remote_copy(
            src_ref=src, dst_ref=dst, send_sem=ssem.at[i], recv_sem=rsem.at[i], device_id=device, device_id_type=MESH
        )

    def send(i, src, dst, device):
        copy = rcopy(i, src, dst, device)
        copy.start()
        sends.append(copy)

    def arrived(i, dst):
        rcopy(i, dst, dst, dev(c_=oc)).wait_recv()

    local = [0]

    def fetch(src, dst):
        i = local[0]
        local[0] += 1
        copy = pltpu.make_async_copy(src, dst, lsem.at[i])
        copy.start()
        return copy

    small = [fetch(tok_h, tok_v), fetch(gain_h, gain_v), fetch(bias_h, bias_v)]

    barrier = pltpu.get_barrier_semaphore()
    peers = [dev(x_=xx(dx), c_=lax.rem(c + dc, NC)) for dx, dc in tpeers]
    peers += [dev(y_=yy(d)) for d in ORDER4] + [dev(z_=zz(d)) for d in ORDER8]
    for p in peers:
        pl.semaphore_signal(barrier, inc=1, device_id=p, device_id_type=MESH)

    def lanes(t):
        return pl.ds(t * 128, 128)

    gate_c = [fetch(gate_h.at[:, :, lanes(t)], gate_r.at[t]) for t in range(NLT)]
    up_c = [fetch(up_h.at[:, :, lanes(t)], up_r.at[t]) for t in range(NLT)]
    down_c = [fetch(down_h.at[:, :, lanes(t)], down_r.at[t]) for t in range(NLT)]
    w4_c = [fetch(w, w4.at[:, pl.ds(512 * i, 512)]) for i, w in enumerate((wq_h, wf_h, wi_h, wo_h))]
    late_c = [fetch(lb_h, lb_v), fetch(hg_h, hg_v), fetch(state_h, st_v), fetch(outw_h, outw_v)]

    for copy in small:
        copy.wait()
    place_t = onehot(iota((128, 16), 0) == tp * 16 + iota((128, 16), 1))
    place = onehot(iota((16, 128), 1) == tp * 16 + iota((16, 128), 0))
    row, col = iota((64, 64), 0), iota((64, 64), 1)
    perm = onehot(col == lax.shift_right_logical(row & 15, 1) * 8 + lax.shift_right_logical(row, 4) * 2 + (row & 1))
    turned = nn_dot(place_t, tok_v[...]).astype(BF)
    token_rows = nt_dot(perm, turned)
    g8[...] = jnp.zeros((8, 128), F32)
    gains = nn_dot(gain_v[...], place)
    biases = nn_dot(bias_v[...], place)
    for i in range(3):
        g8[2 * i : 2 * i + 1, :] = gains[i : i + 1]
        g8[2 * i + 1 : 2 * i + 2, :] = biases[i : i + 1]
    for t in range(NT):
        ts[t] = jnp.concatenate([token_rows[8 * t : 8 * t + 8], g8[...]], axis=0).astype(BF)

    pl.semaphore_wait(barrier, len(peers))

    base = slot(7)
    for i, (dx, dc) in enumerate(tpeers):
        x_, c_ = xx(dx), lax.rem(c + dc, NC)
        send(base + i, ts.at[x_ * NC + c_], tr.at[i], dev(x_=x_, c_=c_))

    def relaid(copies, raw, flat):
        for copy in copies:
            copy.wait()

        def body(t, carry):
            flat[:, pl.ds(pl.multiple_of(t * 128, 128), 128)] = raw[t].reshape(88, 128)
            return carry

        lax.fori_loop(0, NLT, body, 0)

    tile = f32(ts[tp])
    for i in range(7):
        arrived(base + i, tr.at[i])
        tile = tile + f32(tr[i])
    xg[x, c, y, z] = tile[:8].astype(BF)
    gt[y, z] = tile[8:].astype(BF)

    base, gbase = slot(7), slot(7)
    for i, d in enumerate(ORDER8):
        send(base + i, xg.at[x, c, y, z], xg.at[x, c, y, z], dev(z_=zz(d)))
    for i, d in enumerate(ORDER8):
        send(gbase + i, gt.at[y, z], gt.at[y, z], dev(z_=zz(d)))
    relaid(gate_c, gate_r, w2g)
    relaid(up_c, up_r, w2u)
    for i, d in enumerate(ORDER8):
        arrived(base + i, xg.at[x, c, y, zz(NZ - d)])

    ybase, xbase, cbase = slot(3), slot(12), slot(16)
    for i, d in enumerate(ORDER4):
        send(ybase + i, xg.at[x, c, y], xg.at[x, c, y], dev(y_=yy(d)))

    def forward(k, dy):
        yb = yy(NY - dy) if dy else y
        for i, d in enumerate(ORDER4):
            send(xbase + 3 * k + i, xg.at[x, c, yb], xg.at[x, c, yb], dev(x_=xx(d)))
        send(cbase + 4 * k + 3, xg.at[x, c, yb], xg.at[x, c, yb], dev(c_=oc))

    forward(0, 0)
    for i, d in enumerate(ORDER8):
        arrived(gbase + i, gt.at[y, zz(NZ - d)])
    gybase = slot(3)
    for i, d in enumerate(ORDER4):
        send(gybase + i, gt.at[y], gt.at[y], dev(y_=yy(d)))
    for copy in w4_c:
        copy.wait()
    gw = nn_dot(gt[y, z], w4[...])
    gws[...] = gw[:2].astype(BF)
    wbase = slot(3)
    for i, d in enumerate(ORDER4):
        send(wbase + i, gws, gwr.at[i], dev(y_=yy(d)))
    for k, d in enumerate((1, 3, 2)):
        arrived(ybase + ORDER4.index(d), xg.at[x, c, yy(NY - d)])
        forward(k + 1, d)
    relaid(down_c, down_r, d2)
    for k, dy in enumerate((0, 1, 3, 2)):
        yb = yy(NY - dy) if dy else y
        for i, d in enumerate((1, 3, 2)):
            xb = xx(NX - d)
            arrived(xbase + 3 * k + ORDER4.index(d), xg.at[xb, c, yb])
            send(cbase + 4 * k + i, xg.at[xb, c, yb], xg.at[xb, c, yb], dev(c_=oc))
    for k, dy in enumerate((0, 1, 3, 2)):
        yb = yy(NY - dy) if dy else y
        for i, d in enumerate((1, 3, 2)):
            arrived(cbase + 4 * k + i, xg.at[xx(NX - d), oc, yb])
        arrived(cbase + 4 * k + 3, xg.at[x, oc, yb])

    def ffn(whole, which, put):
        gate = nt_dot(whole, w2g[...])
        up = nt_dot(whole, w2u[...])
        hidden = jax.nn.silu(gate) * up
        hidden = jnp.where((iota(hidden.shape, 1) & 1) == which, hidden, 0.0).astype(BF)
        for zb_ in range(NZ):
            part = nn_dot(hidden, d2[:, 512 * zb_ : 512 * zb_ + 512])
            for yb_ in range(NY):
                for t in range(NT):
                    put(t // NC, t % NC, yb_, zb_, part[8 * t : 8 * t + 8, 128 * yb_ : 128 * yb_ + 128].astype(BF))

    def over_core_and_x(s, r, t, rr, u):
        cb, xb_ = slot(4), slot(3)
        for i, d in enumerate((2, 1, 3, 0)):
            x_ = xx(d)
            send(cb + i, s.at[oc, x_], r.at[x_], dev(c_=oc))
        for i, d in enumerate((2, 1, 3)):
            x_ = xx(d)
            arrived(cb + i, r.at[x_])
            t[i] = (f32(s[c, x_]) + f32(r[x_])).astype(BF)
            send(xb_ + i, t.at[i], rr.at[i], dev(x_=x_))
        arrived(cb + 3, r.at[x])
        u[...] = f32(s[c, x]) + f32(r[x])
        for i in range(3):
            arrived(xb_ + i, rr.at[i])
        u[...] = u[...] + f32(rr[0]) + f32(rr[1]) + f32(rr[2])

    whole = jnp.concatenate([xg[:, :, k % NY, k // NY].reshape(64, 128) for k in range(NLT)], axis=1)

    def put0(x_, c_, y_, z_, v):
        s0[c_, x_, y_, z_] = v

    ffn(whole, 0, put0)
    over_core_and_x(s0, r0, t0, r1, u0)
    base = slot(3)
    for i, d in enumerate(ORDER4):
        v0[i] = u0[yy(d)].astype(BF)
        send(base + i, v0.at[i], r2.at[i], dev(y_=yy(d)))
    w0[...] = u0[y]
    for i, d in enumerate(ORDER4):
        arrived(gybase + i, gt.at[yy(NY - d)])
    gw = f32(gws[...])
    for i in range(3):
        arrived(wbase + i, gwr.at[i])
        gw = gw + f32(gwr[i])
    gws2[...] = gw.astype(BF)
    wzbase = slot(7)
    for i, d in enumerate(ORDER8):
        send(wzbase + i, gws2, gwr2.at[i], dev(z_=zz(d)))
    own_tok = f32(xg[x, c])
    shift = RES * jnp.sum(jnp.sum(own_tok, axis=(0, 1)), axis=1, keepdims=True) * (1.0 / D)
    for i in range(3):
        arrived(base + i, r2.at[i])
    w0[...] = w0[...] + f32(r2[0]) + f32(r2[1]) + f32(r2[2])
    base = slot(7)
    for i, d in enumerate(ORDER8):
        q0[i] = w0[zz(d)].astype(BF)
        send(base + i, q0.at[i], r3.at[i], dev(z_=zz(d)))
    total = w0[z]
    for i in range(7):
        arrived(base + i, r3.at[i])
        total = total + f32(r3[i])
    zb[tp] = (RES * f32(xg[x, c, y, z]) + 0.5 * total - shift).astype(BF)
    base = slot(7)
    for i, (dx, dc) in enumerate(tpeers):
        send(base + i, zb.at[tp], zb.at[tp], dev(x_=xx(dx), c_=lax.rem(c + dc, NC)))
    for i, (dx, dc) in enumerate(tpeers):
        from_x, from_c = xx(NX - dx) if dx else x, lax.rem(c + dc, NC)
        arrived(base + i, zb.at[from_x * NC + from_c])

    zv = f32(zb[...].reshape(64, 128))
    mine = f32(gt[y, z])
    proj = nn_dot((zv * mine[0:1]).astype(BF), w4[...])
    for y_ in range(NY):
        se[y_] = proj[16 * y_ : 16 * y_ + 16].astype(BF)
    base = slot(3)
    for i, d in enumerate(ORDER4):
        send(base + i, se.at[yy(d)], re.at[i], dev(y_=yy(d)))
    sums = jnp.where(
        iota((64, 128), 1) < 64,
        jnp.sum(zv, axis=1, keepdims=True),
        jnp.sum(zv * zv, axis=1, keepdims=True),
    )
    for y_ in range(NY):
        st[y_] = sums[16 * y_ : 16 * y_ + 16]
        rzs[y_] = zv[16 * y_ : 16 * y_ + 16].astype(BF)
    sbase, rbase = slot(3), slot(3)
    for i, d in enumerate(ORDER4):
        send(sbase + i, st.at[yy(d)], rst.at[i], dev(y_=yy(d)))
        send(rbase + i, rzs.at[yy(d)], rz.at[y], dev(y_=yy(d)))
    rz[y] = rzs[y]
    gwv = f32(gws2[...])
    for i in range(7):
        arrived(wzbase + i, gwr2.at[i])
        gwv = gwv + f32(gwr2[i])
    gwt[...] = gwv
    for copy in late_c:
        copy.wait()
    acc = f32(se[y])
    for i in range(3):
        arrived(base + i, re.at[i])
        acc = acc + f32(re[i])
    sz[...] = acc.reshape(NZ, 2, 2048).astype(BF)
    base = slot(7)
    for i, d in enumerate(ORDER8):
        send(base + i, sz.at[zz(d)], rze.at[i], dev(z_=zz(d)))
    acc = st[y]
    for i in range(3):
        arrived(sbase + i, rst.at[i])
        acc = acc + rst[i]
    szs[...] = acc.reshape(NZ, 2, 128)
    for i, d in enumerate(ORDER4):
        arrived(rbase + i, rz.at[yy(NY - d)])
    resid = jnp.concatenate([f32(rz[y_]) for y_ in range(NY)], axis=1)
    rz2s = resid.reshape(NZ, 2, 512).astype(BF)
    sv[...] = rz2s
    sbase, rbase = slot(7), slot(7)
    for i, d in enumerate(ORDER8):
        send(sbase + i, szs.at[zz(d)], rzst.at[i], dev(z_=zz(d)))
        send(rbase + i, sv.at[zz(d)], rz2.at[z], dev(z_=zz(d)))
    rz2[z] = sv[z]
    acc = f32(sz[z])
    for i in range(7):
        arrived(base + i, rze.at[i])
        acc = acc + f32(rze[i])
    stat = szs[z]
    for i in range(7):
        arrived(sbase + i, rzst.at[i])
        stat = stat + rzst[i]
    for i, d in enumerate(ORDER8):
        arrived(rbase + i, rz2.at[zz(NZ - d)])
    mean = stat[:, 0:1] * (1.0 / D)
    var = jnp.maximum(stat[:, 64:65] * (1.0 / D) - mean * mean, 0.0)
    scale = lax.rsqrt(var + NORM_EPS)
    proj = (scale * (acc - mean * gwt[0:1]) + gwt[1:2]).astype(BF).astype(F32)

    def by_head(v):
        return jnp.concatenate([v[:, 128 * h : 128 * h + 128] for h in range(4)], axis=0)

    def twice(v):
        return jnp.concatenate([v[h : h + 1] for h in range(4) for _ in range(2)], axis=0)

    query_pre, forget_pre = by_head(proj[:, :512]), by_head(proj[:, 512:1024])
    input_pre, outgate_pre = by_head(proj[:, 1024:1536]), by_head(proj[:, 1536:])
    low, head_gain = twice(lb_v[...]), twice(hg_v[...])
    forget = low + (1.0 - low) * jax.nn.sigmoid(forget_pre)
    key_part = (1.0 - low) * jax.nn.sigmoid(-forget_pre)
    forget_t, key_t, query_t = forget.T, key_part.T, jax.nn.silu(query_pre).T
    reads = []
    for h in range(4):
        for s in range(2):
            i = 2 * h + s
            updated = forget_t[:, i : i + 1] * st_v[s, h] + key_t[:, i : i + 1] * input_pre[i : i + 1]
            ns_v[s, h] = updated
            reads.append(jnp.sum(query_t[:, i : i + 1] * updated, axis=0, keepdims=True))
    ns_copy = fetch(ns_v, ns_h)
    readout = jnp.concatenate(reads, axis=0)
    readout = readout * lax.rsqrt(jnp.mean(readout * readout, axis=1, keepdims=True) + HEAD_EPS)
    gated = readout * head_gain * jax.nn.silu(outgate_pre)
    gated = jnp.concatenate([gated[2 * h : 2 * h + 2] for h in range(4)], axis=1).astype(BF)
    for t in range(NT):
        sf[t] = nn_dot(gated, outw_v[:, 512 * t : 512 * t + 512]).astype(BF)
    base = slot(7)
    for i, (dx, dc) in enumerate(tpeers):
        x_, c_ = xx(dx), lax.rem(c + dc, NC)
        send(base + i, sf.at[x_ * NC + c_], rf.at[i], dev(x_=x_, c_=c_))
    gain_row = jnp.concatenate([f32(gt[y_, tp])[0:1] for y_ in range(NY)], axis=1)
    bias_row = jnp.concatenate([f32(gt[y_, tp])[1:2] for y_ in range(NY)], axis=1)
    normed_one = ((f32(rz2[tp]) - mean) * scale * gain_row + bias_row).astype(BF)
    mix = f32(sf[tp])
    for i in range(7):
        arrived(base + i, rf.at[i])
        mix = mix + f32(rf[i])
    yz[z] = (RES * f32(normed_one) + mix).astype(BF)

    base = slot(7)
    for i, d in enumerate(ORDER8):
        send(base + i, yz.at[z], yz.at[z], dev(z_=zz(d)))
    for i, d in enumerate(ORDER8):
        arrived(base + i, yz.at[zz(NZ - d)])
    yg[x, c, y] = f32(yz[...]).reshape(16, 512).astype(BF)
    ybase, xbase, cbase = slot(3), slot(12), slot(16)
    for i, d in enumerate(ORDER4):
        send(ybase + i, yg.at[x, c, y], yg.at[x, c, y], dev(y_=yy(d)))

    def forward2(k, dy):
        yb = yy(NY - dy) if dy else y
        for i, d in enumerate(ORDER4):
            send(xbase + 3 * k + i, yg.at[x, c, yb], yg.at[x, c, yb], dev(x_=xx(d)))
        send(cbase + 4 * k + 3, yg.at[x, c, yb], yg.at[x, c, yb], dev(c_=oc))

    forward2(0, 0)
    for k, d in enumerate((1, 3, 2)):
        arrived(ybase + ORDER4.index(d), yg.at[x, c, yy(NY - d)])
        forward2(k + 1, d)
    for k, dy in enumerate((0, 1, 3, 2)):
        yb = yy(NY - dy) if dy else y
        for i, d in enumerate((1, 3, 2)):
            xb = xx(NX - d)
            arrived(xbase + 3 * k + ORDER4.index(d), yg.at[xb, c, yb])
            send(cbase + 4 * k + i, yg.at[xb, c, yb], yg.at[xb, c, yb], dev(c_=oc))
    for k, dy in enumerate((0, 1, 3, 2)):
        yb = yy(NY - dy) if dy else y
        for i, d in enumerate((1, 3, 2)):
            arrived(cbase + 4 * k + i, yg.at[xx(NX - d), oc, yb])
        arrived(cbase + 4 * k + 3, yg.at[x, oc, yb])

    streams = [f32(yg[t // NC, t % NC].reshape(64, 512)) for t in range(NT)]
    mean = sum(jnp.sum(v, axis=1, keepdims=True) for v in streams) * (1.0 / D)
    streams = [v - mean for v in streams]
    var = sum(jnp.sum(v * v, axis=1, keepdims=True) for v in streams) * (1.0 / D)
    scale = lax.rsqrt(var + NORM_EPS)
    normed = []
    for t in range(NT):
        gain_row = jnp.concatenate([f32(gt[y_, t])[2:3] for y_ in range(NY)], axis=1)
        bias_row = jnp.concatenate([f32(gt[y_, t])[3:4] for y_ in range(NY)], axis=1)
        normed.append((streams[t] * scale * gain_row + bias_row).astype(BF))
        for y_ in range(NY):
            xn[t, y_] = normed[t][:, 128 * y_ : 128 * y_ + 128].reshape(NT, 8, 128)
    whole = jnp.concatenate(normed, axis=1)

    def put1(x_, c_, y_, z_, v):
        s1[c_, x_, z_, y_] = v

    ffn(whole, 1, put1)
    over_core_and_x(s1, r0b, t1, r1b, u1)
    base = slot(7)
    for i, d in enumerate(ORDER8):
        v1[i] = u1[zz(d)].astype(BF)
        send(base + i, v1.at[i], r2b.at[i], dev(z_=zz(d)))
    w1[...] = u1[z]
    for i in range(7):
        arrived(base + i, r2b.at[i])
        w1[...] = w1[...] + f32(r2b[i])
    q1[...] = w1[...].astype(BF)
    base = slot(3)
    for i, d in enumerate(ORDER4):
        send(base + i, q1, r3b.at[i], dev(y_=yy(d)))
    resid = jnp.concatenate([RES * f32(xn[z, y_, tp]) for y_ in range(NY)], axis=1)
    for i in range(3):
        arrived(base + i, r3b.at[i])
    total = f32(q1[...]) + f32(r3b[0]) + f32(r3b[1]) + f32(r3b[2])
    total = jnp.concatenate([total[y_] for y_ in range(NY)], axis=1)
    stream = resid + 0.5 * total
    for y_ in range(NY):
        w1[y_] = stream[:, 128 * y_ : 128 * y_ + 128]
    rv[tp] = w1[y]
    vbase = slot(7)
    for i, (dx, dc) in enumerate(tpeers):
        send(vbase + i, rv.at[tp], rv.at[tp], dev(x_=xx(dx), c_=lax.rem(c + dc, NC)))

    part_mean = jnp.sum(stream, axis=1, keepdims=True) * (1.0 / 512)
    centred = stream - part_mean
    part_sq = jnp.sum(centred * centred, axis=1, keepdims=True)
    low_half = iota((8, 128), 1) < 64
    sa[...] = jnp.where(low_half, part_mean, part_sq)
    base = slot(7)
    for i, d in enumerate(ORDER8):
        send(base + i, sa, ra.at[i], dev(z_=zz(d)))
    for i in range(7):
        arrived(base + i, ra.at[i])
    parts = [sa[...]] + [ra[i] for i in range(7)]
    means = [p[:, 0:1] for p in parts]
    mean = sum(means) * (1.0 / NZ)
    sq = sum(p[:, 64:65] for p in parts)
    for m in means:
        sq = sq + 512.0 * (m - mean) * (m - mean)
    rb[tp] = jnp.where(low_half, mean, lax.rsqrt(sq * (1.0 / D) + NORM_EPS))
    base = slot(7)
    for i, (dx, dc) in enumerate(tpeers):
        send(base + i, rb.at[tp], rb.at[tp], dev(x_=xx(dx), c_=lax.rem(c + dc, NC)))
    for i, (dx, dc) in enumerate(tpeers):
        source = (xx(NX - dx) if dx else x) * NC + lax.rem(c + dc, NC)
        arrived(vbase + i, rv.at[source])
        arrived(base + i, rb.at[source])
    values, stats = rv[...].reshape(64, 128), rb[...].reshape(64, 128)
    mine = f32(gt[y, z])
    last = ((values - stats[:, 0:1]) * stats[:, 64:65] * mine[4:5] + mine[5:6]).astype(BF)
    picked = nt_dot(place, last).astype(BF)
    mixed_ref[...] = nn_dot(picked, perm).astype(BF)

    ns_copy.wait()
    for copy in sends:
        copy.wait_send()


def vm(*shape, dtype=BF):
    return pltpu.VMEM(shape, dtype)


def local(
    tokens, gate_weights, up_weights, down_weights, norm_gain, norm_bias, query_weight, forget_weight, input_weight,
    outgate_weight, lower_bound, head_gain, out_weight, state,
):
    hbm = pl.BlockSpec(memory_space=pl.ANY)
    f = F32
    scratch = [
        vm(16, 64), vm(3, 16), vm(3, 16), vm(4, 128, dtype=f), vm(4, 128, dtype=f),
        vm(NLT, 44, 2, 128), vm(NLT, 44, 2, 128), vm(NLT, 44, 2, 128), vm(88, D), vm(88, D), vm(88, D),
        vm(128, 2048), vm(512, D), vm(2, 4, 128, 128, dtype=f), vm(2, 4, 128, 128, dtype=f),
        vm(8, 128, dtype=f), vm(NT, 16, 128), vm(7, 16, 128), vm(NX, NC, NY, NZ, 8, 128), vm(NY, NZ, 8, 128),
        vm(2, 2048), vm(3, 2, 2048), vm(2, 2048), vm(7, 2, 2048), vm(2, 2048, dtype=f),
        vm(NC, NX, NY, NZ, 8, 128), vm(NX, NY, NZ, 8, 128), vm(3, NY, NZ, 8, 128), vm(3, NY, NZ, 8, 128),
        vm(NY, NZ, 8, 128, dtype=f), vm(3, NZ, 8, 128), vm(3, NZ, 8, 128), vm(NZ, 8, 128, dtype=f),
        vm(7, 8, 128), vm(7, 8, 128), vm(NT, 8, 128),
        vm(NY, 16, 2048), vm(NY, 16, 128, dtype=f), vm(NY, 16, 128), vm(3, 16, 2048), vm(3, 16, 128, dtype=f),
        vm(NZ, 2, 2048), vm(NZ, 2, 128, dtype=f), vm(NY, 16, 128), vm(7, 2, 2048), vm(7, 2, 128, dtype=f),
        vm(NZ, 2, 512),
        vm(NT, 2, 512), vm(7, 2, 512), vm(NZ, 2, 512), vm(NX, NC, NY, 16, 512), vm(NZ, NY, NT, 8, 128),
        vm(NC, NX, NZ, NY, 8, 128), vm(NX, NZ, NY, 8, 128), vm(3, NZ, NY, 8, 128), vm(3, NZ, NY, 8, 128),
        vm(NZ, NY, 8, 128, dtype=f), vm(7, NY, 8, 128), vm(7, NY, 8, 128), vm(NY, 8, 128, dtype=f),
        vm(NY, 8, 128), vm(3, NY, 8, 128), vm(8, 128, dtype=f), vm(7, 8, 128, dtype=f), vm(1, 8, 128, dtype=f),
        vm(NT, 8, 128, dtype=f), vm(NZ, 2, 512), vm(NT, 8, 128, dtype=f),
        pltpu.SemaphoreType.DMA((NREMOTE,)), pltpu.SemaphoreType.DMA((NREMOTE,)), pltpu.SemaphoreType.DMA((NLOCAL,)),
    ]
    mixed_t, new_state = pl.pallas_call(
        kernel,
        out_shape=(jax.ShapeDtypeStruct((16, 64), BF), jax.ShapeDtypeStruct(state.shape, F32)),
        in_specs=[hbm] * 14,
        out_specs=(pl.BlockSpec(memory_space=pltpu.VMEM), hbm),
        scratch_shapes=scratch,
        compiler_params=pltpu.CompilerParams(
            collective_id=0, has_side_effects=True, vmem_limit_bytes=48 * 1024 * 1024
        ),
        name="decode_step",
    )(
        tokens.T,
        jnp.transpose(gate_weights, (2, 0, 1)),
        jnp.transpose(up_weights, (2, 0, 1)),
        jnp.transpose(down_weights, (1, 0, 2)),
        norm_gain,
        norm_bias,
        query_weight,
        forget_weight,
        input_weight,
        outgate_weight,
        lower_bound.reshape(4, 128),
        head_gain.reshape(4, 128),
        out_weight,
        state,
    )
    return mixed_t.T, new_state


def solution(mesh):
    both = ("kv", "tp")
    in_specs = (
        P(None, both), P(None, None, both), P(None, None, both), P(None, both, None), P(None, both), P(None, both),
        P("kv", "tp"), P("kv", "tp"), P("kv", "tp"), P("kv", "tp"), P("tp"), P("tp"), P("tp", None),
        P("kv", "tp", None, None),
    )
    out_specs = (P(None, both), P("kv", "tp", None, None))
    return jax.shard_map(local, mesh=mesh, in_specs=in_specs, out_specs=out_specs, check_vma=False)
```

```python
import jax
import jax.numpy as jnp
from jax import lax
from jax.experimental import pallas as pl
from jax.experimental.pallas import tpu as pltpu
from jax.sharding import PartitionSpec as P

MESH = pl.DeviceIdType.MESH
BF = jnp.bfloat16
F32 = jnp.float32
NZ, NY, NX, NC = 8, 4, 4, 2
NT = NX * NC
D = 4096
HEAD = 128
NLT = D // 128
RES = 8.0**0.25
NORM_EPS = 1e-05
HEAD_EPS = 1e-06
ORDER8 = (4, 3, 5, 2, 6, 1, 7)
ORDER4 = (2, 1, 3)
NREMOTE = 80
NLOCAL = 11


def nt_dot(a, b):
    return lax.dot_general(a, b, (((1,), (1,)), ((), ())), preferred_element_type=F32)


def nn_dot(a, b):
    return jnp.dot(a, b, preferred_element_type=F32)


def iota(shape, dim):
    return lax.broadcasted_iota(jnp.int32, shape, dim)


def onehot(mask):
    return jnp.where(mask, 1.0, 0.0).astype(BF)


def f32(v):
    return v.astype(F32)


def kernel(
    tok_h, gate_h, up_h, down_h, gain_h, bias_h, wq_h, wf_h, wi_h, wo_h, lb_h, hg_h, outw_h, state_h,
    mixed_ref, ns_ref,
    tok_v, gain_v, bias_v, lb_v, hg_v, gate_r, up_r, down_r, w2g, w2u, d2, wl, w4, outw_v, st_v,
    g8, ts, tr, xg, gt, gws, gwr, gws2, gwr2, gwt,
    s0, r0, t0, r1, u0, v0, r2, w0, q0, r3, zb, tok_s, shift_s,
    se, st, rz, re, rst, sz, szs, rzs, rze, rzst, rz2,
    sf, rf, yz, yg, xn,
    s1, r0b, t1, r1b, u1, v1, r2b, w1, q1, r3b, sa, ra, rb, sv, rv,
    ssem, rsem, lsem,
):
    kv = lax.axis_index("kv")
    tp = lax.axis_index("tp")
    z, y = lax.div(kv, NY), lax.rem(kv, NY)
    x, c = lax.div(tp, NC), lax.rem(tp, NC)

    oc = 1 - c

    def dev(z_=None, y_=None, x_=None, c_=None):
        z_, y_ = z if z_ is None else z_, y if y_ is None else y_
        x_, c_ = x if x_ is None else x_, c if c_ is None else c_
        return (z_ * NY + y_, x_ * NC + c_)

    def zz(d):
        return lax.rem(z + d, NZ)

    def yy(d):
        return lax.rem(y + d, NY)

    def xx(d):
        return lax.rem(x + d, NX)

    tpeers = [(dx, dc) for dc in (1, 0) for dx in (2, 1, 3, 0) if (dx, dc) != (0, 0)]

    inner, outer = y * oc + x * c, x * oc + y * c

    def step_inner(d):
        return lax.rem(inner + d, 4), dev(y_=lax.rem(y + d * oc, NY), x_=lax.rem(x + d * c, NX))

    def step_outer(d):
        return lax.rem(outer + d, 4), dev(y_=lax.rem(y + d * c, NY), x_=lax.rem(x + d * oc, NX))

    finals = []
    count = [0]

    def slot(n=1):
        first = count[0]
        count[0] += n
        assert count[0] <= NREMOTE
        return first

    def rcopy(i, j, src, dst, device):
        return pltpu.make_async_remote_copy(
            src_ref=src, dst_ref=dst, send_sem=ssem.at[i], recv_sem=rsem.at[j], device_id=device, device_id_type=MESH
        )

    def send(i, j, src, dst, device):
        rcopy(i, j, src, dst, device).start()

    def arrived(j, like):
        rcopy(j, j, like, like, dev(c_=oc)).wait_recv()

    def stage(copies, like):
        i = slot()
        for src, dst, device in copies:
            send(i, i, src, dst, device)
        finals.append((i, like))
        return i

    nlocal = [0]

    def fetch(pairs, like=None):
        i = nlocal[0]
        nlocal[0] += 1
        for src, dst in pairs:
            copy = pltpu.make_async_copy(src, dst, lsem.at[i])
            copy.start()
        return copy if like is None else pltpu.make_async_copy(like, like, lsem.at[i])

    tok_c = fetch([(tok_h, tok_v)])
    gain_c = [fetch([(gain_h, gain_v)]), fetch([(bias_h, bias_v)])]

    barrier = pltpu.get_barrier_semaphore()
    peers = [dev(x_=xx(dx), c_=lax.rem(c + dc, NC)) for dx, dc in tpeers]
    peers += [dev(y_=yy(d)) for d in ORDER4] + [dev(z_=zz(d)) for d in ORDER8]
    for p in peers:
        pl.semaphore_signal(barrier, inc=1, device_id=p, device_id_type=MESH)

    def lanes(t):
        return pl.ds(t * 128, 128)

    gate_c = fetch([(gate_h.at[:, :, lanes(t)], gate_r.at[t]) for t in range(NLT)], gate_r)
    up_c = fetch([(up_h.at[:, :, lanes(t)], up_r.at[t]) for t in range(NLT)], up_r)
    down_c = fetch([(down_h.at[:, :, lanes(t)], down_r.at[t]) for t in range(NLT)], down_r)
    w4_c = fetch([(w, w4.at[:, pl.ds(512 * i, 512)]) for i, w in enumerate((wq_h, wf_h, wi_h, wo_h))], w4)
    late_c = [fetch([(lb_h, lb_v)]), fetch([(hg_h, hg_v)]), fetch([(state_h, st_v)]), fetch([(outw_h, outw_v)])]

    tok_c.wait()
    row, col = iota((128, 64), 0) & 63, iota((128, 64), 1)
    perm2 = onehot(col == lax.shift_right_logical(row & 15, 1) * 8 + lax.shift_right_logical(row, 4) * 2 + (row & 1))
    turned = nt_dot(tok_v[...], perm2)
    xg[c, outer, inner, z] = jnp.where(iota((8, 128), 1) < 64, turned[:8], turned[8:]).astype(BF)
    for copy in gain_c:
        copy.wait()
    place = onehot(iota((16, 128), 1) == tp * 16 + iota((16, 128), 0))
    g8[...] = jnp.zeros((8, 128), F32)
    gains = nn_dot(gain_v[...], place)
    biases = nn_dot(bias_v[...], place)
    for i in range(3):
        g8[2 * i : 2 * i + 1, :] = gains[i : i + 1]
        g8[2 * i + 1 : 2 * i + 2, :] = biases[i : i + 1]
    ts[...] = g8[...].astype(BF)

    lane_in, lane_out = iota((256, 256), 0), iota((256, 256), 1)
    low8, mid, high = lane_in & 7, lax.shift_right_logical(lane_in, 4), lax.shift_right_logical(lane_in, 3) & 1
    shuffle = onehot(lane_out == high * 128 + mid * 8 + low8)
    zeros8 = jnp.zeros((8, 2048), BF)
    for i in range(4):
        wl[96 * i + 88 : 96 * i + 96, :] = zeros8

    def relaid(raw, flat, at):
        for t in range(NLT // 2):
            both = jnp.concatenate([raw[2 * t].reshape(88, 128), raw[2 * t + 1].reshape(88, 128)], axis=1)
            flat[:, 256 * t : 256 * t + 256] = both
            if at is not None:
                moved = nn_dot(both, shuffle).astype(BF)
                wl[at : at + 88, 128 * t : 128 * t + 128] = moved[:, :128]
                wl[at + 96 : at + 184, 128 * t : 128 * t + 128] = moved[:, 128:]

    gate_c.wait()
    relaid(gate_r, w2g, 0)

    pl.semaphore_wait(barrier, len(peers))

    own = xg.at[c, outer, inner, z]
    zs = stage([(own, own, dev(z_=zz(d))) for d in ORDER8], r3)
    gs = stage([(ts, tr.at[i], dev(x_=xx(dx), c_=lax.rem(c + dc, NC))) for i, (dx, dc) in enumerate(tpeers)], r3)
    up_c.wait()
    relaid(up_r, w2u, 192)
    arrived(zs, r3)

    def spread(buf, like3, like16):
        ab, bb, cs = slot(3), slot(4), slot()
        mine = buf.at[c, outer, inner]
        for i, d in enumerate(ORDER4):
            send(ab, ab + i, mine, mine, step_inner(d)[1])
        finals.append((ab, like3))

        def forward(k, at):
            block = buf.at[c, outer, at]
            for d in ORDER4:
                send(bb + k, bb + k, block, block, step_outer(d)[1])
            finals.append((bb + k, like3))
            send(cs, cs, block, block, dev(c_=oc))

        forward(0, inner)
        yield
        order = (1, 3, 2)
        for k, d in enumerate(order):
            at = step_inner(4 - d)[0]
            arrived(ab + ORDER4.index(d), buf.at[c, outer, at])
            forward(k + 1, at)
        yield
        for k, d in enumerate((0, *order)):
            at = step_inner(4 - d)[0] if d else inner
            arrived(bb + k, like3)
            for e in (1, 2, 3):
                block = buf.at[c, step_outer(e)[0], at]
                send(cs, cs, block, block, dev(c_=oc))
        finals.append((cs, like16))
        arrived(cs, like16)
        yield

    gather = spread(xg, r2, r0)
    next(gather)
    arrived(gs, r3)
    tile = f32(ts[...])
    for i in range(7):
        tile = tile + f32(tr[i])
    gt[y, z] = tile.astype(BF)
    own = gt.at[y, z]
    gs = stage([(own, own, dev(z_=zz(d))) for d in ORDER8], r3)
    next(gather)
    w4_c.wait()
    gw = nn_dot(gt[y, z], w4[...])
    gws[...] = gw[:2].astype(BF)
    ws = stage([(gws, gwr.at[i], dev(y_=yy(d))) for i, d in enumerate(ORDER4)], gwr)
    down_c.wait()
    relaid(down_r, d2, None)
    next(gather)

    def down(hidden, put):
        for zb_ in range(NZ):
            part = nn_dot(hidden, d2[:, 512 * zb_ : 512 * zb_ + 512])
            for yb_ in range(NY):
                for t in range(NT):
                    put(t // NC, t % NC, yb_, zb_, part[8 * t : 8 * t + 8, 128 * yb_ : 128 * yb_ + 128].astype(BF))

    def over_core_and(s, r, t, rr, u, me, theirs, step):
        cb, cs, ps = slot(3), slot(), slot()
        at = [(cb, 2), (cb + 1, 1), (cb + 2, 3), (cs, 0)]
        for j, d in at:
            p = lax.rem(theirs + d, 4)
            send(cs, j, s.at[oc, p], r.at[p], dev(c_=oc))
        finals.append((cs, r))
        for i, (j, d) in enumerate(at[:3]):
            p, device = step(d)
            arrived(j, r.at[p])
            t[i] = (f32(s[c, p]) + f32(r[p])).astype(BF)
            send(ps, ps, t.at[i], rr.at[i], device)
        finals.append((ps, rr))
        arrived(cs, r.at[me])
        u[...] = f32(s[c, me]) + f32(r[me])
        arrived(ps, rr)
        u[...] = u[...] + f32(rr[0]) + f32(rr[1]) + f32(rr[2])

    def halves(first):
        return first[0:88, 0:64] + first[96:184, 64:128]

    tiles = [xg[0, x_, y_, z_] if c_ == 0 else xg[1, y_, x_, z_]
             for z_ in range(NZ) for y_ in range(NY) for x_ in range(NX) for c_ in range(NC)]
    whole = jnp.concatenate(tiles, axis=0)
    both = nn_dot(wl[...], whole)
    hidden = jax.nn.silu(halves(both[:192])) * halves(both[192:])
    hidden = jnp.where((iota(hidden.shape, 0) & 1) == 0, hidden, 0.0).T.astype(BF)

    def put0(x_, c_, y_, z_, v):
        if c_ == 0:
            s0[0, x_, y_, z_] = v
        else:
            s0[1, y_, x_, z_] = v

    down(hidden, put0)
    over_core_and(s0, r0, t0, r1, u0, outer, inner, step_outer)
    copies = []
    for i, d in enumerate(ORDER4):
        at, device = step_inner(d)
        v0[i] = u0[at].astype(BF)
        copies.append((v0.at[i], r2.at[i], device))
    rs = stage(copies, r2)
    w0[...] = u0[inner]
    arrived(gs, r3)
    own = gt.at[y]
    gs = stage([(own, own, dev(y_=yy(d))) for d in ORDER4], r2)
    arrived(ws, gwr)
    gw = f32(gws[...])
    for i in range(3):
        gw = gw + f32(gwr[i])
    gws2[...] = gw.astype(BF)
    ws = stage([(gws2, gwr2.at[i], dev(z_=zz(d))) for i, d in enumerate(ORDER8)], gwr2)
    line = jnp.sum(f32(whole).reshape(256, 8, 128), axis=0)
    line = jnp.sum(line, axis=0, keepdims=True) * (RES / D)
    line = line[:, :64] + line[:, 64:]
    shift_s[...] = jnp.broadcast_to(jnp.broadcast_to(line, (8, 64)).T[:, 0:1], (64, 128)).reshape(NT, 8, 128)
    pieces = []
    for m in range(NT):
        piece = f32(xg[0, m // NC, y, z] if m % NC == 0 else xg[1, y, m // NC, z])
        pieces += [piece[:, :64], piece[:, 64:]]
    tok_s[...] = jnp.concatenate(pieces, axis=0).T.reshape(NT, 8, 128)
    base_tile = RES * tok_s[tp] - shift_s[tp]
    arrived(rs, r2)
    w0[...] = w0[...] + f32(r2[0]) + f32(r2[1]) + f32(r2[2])
    copies = []
    for i, d in enumerate(ORDER8):
        q0[i] = w0[zz(d)].astype(BF)
        copies.append((q0.at[i], r3.at[i], dev(z_=zz(d))))
    rs = stage(copies, r3)
    total = w0[z]
    arrived(rs, r3)
    for i in range(7):
        total = total + f32(r3[i])
    zb[tp] = (base_tile + 0.5 * total).astype(BF)
    own = zb.at[tp]
    rs = stage([(own, own, dev(x_=xx(dx), c_=lax.rem(c + dc, NC))) for dx, dc in tpeers], r3)
    arrived(rs, r3)

    def by_head(v):
        return jnp.concatenate([v[:, 128 * h : 128 * h + 128] for h in range(4)], axis=0)

    def twice(v):
        return jnp.concatenate([v[h : h + 1] for h in range(4) for _ in range(2)], axis=0)

    zv = f32(zb[...].reshape(64, 128))
    mine = f32(gt[y, z])
    proj = nn_dot((zv * mine[0:1]).astype(BF), w4[...])
    for y_ in range(NY):
        se[y_] = proj[16 * y_ : 16 * y_ + 16].astype(BF)
    es = stage([(se.at[yy(d)], re.at[i], dev(y_=yy(d))) for i, d in enumerate(ORDER4)], re)
    sums = jnp.where(
        iota((64, 128), 1) < 64,
        jnp.sum(zv, axis=1, keepdims=True),
        jnp.sum(zv * zv, axis=1, keepdims=True),
    )
    for y_ in range(NY):
        st[y_] = sums[16 * y_ : 16 * y_ + 16]
        rzs[y_] = zv[16 * y_ : 16 * y_ + 16].astype(BF)
    fs = stage([(st.at[yy(d)], rst.at[i], dev(y_=yy(d))) for i, d in enumerate(ORDER4)], rst)
    hs = stage([(rzs.at[yy(d)], rz.at[y], dev(y_=yy(d))) for i, d in enumerate(ORDER4)], rz.at[0:3])
    rz[y] = rzs[y]
    arrived(gs, r2)
    arrived(ws, gwr2)
    gwv = f32(gws2[...])
    for i in range(7):
        gwv = gwv + f32(gwr2[i])
    gwt[...] = gwv
    for copy in late_c:
        copy.wait()
    arrived(es, re)
    acc = f32(se[y]) + f32(re[0]) + f32(re[1]) + f32(re[2])
    sz[...] = acc.reshape(NZ, 2, 2048).astype(BF)
    es = stage([(sz.at[zz(d)], rze.at[i], dev(z_=zz(d))) for i, d in enumerate(ORDER8)], rze)
    arrived(fs, rst)
    acc = st[y] + rst[0] + rst[1] + rst[2]
    szs[...] = acc.reshape(NZ, 2, 128)
    fs = stage([(szs.at[zz(d)], rzst.at[i], dev(z_=zz(d))) for i, d in enumerate(ORDER8)], rzst)
    arrived(hs, rz.at[0:3])
    resid = jnp.concatenate([f32(rz[y_]) for y_ in range(NY)], axis=1)
    sv[...] = resid.reshape(NZ, 2, 512).astype(BF)
    hs = stage([(sv.at[zz(d)], rz2.at[z], dev(z_=zz(d))) for i, d in enumerate(ORDER8)], rz2.at[0:7])
    rz2[z] = sv[z]
    low, head_gain = twice(lb_v[...]), twice(hg_v[...])
    gain_row = jnp.concatenate([f32(gt[y_, tp])[0:1] for y_ in range(NY)], axis=1)
    bias_row = jnp.concatenate([f32(gt[y_, tp])[1:2] for y_ in range(NY)], axis=1)
    arrived(fs, rzst)
    stat = szs[z]
    for i in range(7):
        stat = stat + rzst[i]
    mean = stat[:, 0:1] * (1.0 / D)
    var = jnp.maximum(stat[:, 64:65] * (1.0 / D) - mean * mean, 0.0)
    scale = lax.rsqrt(var + NORM_EPS)
    arrived(es, rze)
    acc = f32(sz[z])
    for i in range(7):
        acc = acc + f32(rze[i])
    proj = (scale * (acc - mean * gwt[0:1]) + gwt[1:2]).astype(BF).astype(F32)

    query_pre, forget_pre = by_head(proj[:, :512]), by_head(proj[:, 512:1024])
    input_pre, outgate_pre = by_head(proj[:, 1024:1536]), by_head(proj[:, 1536:])
    forget = low + (1.0 - low) * jax.nn.sigmoid(forget_pre)
    key_part = (1.0 - low) * jax.nn.sigmoid(-forget_pre)
    forget_t, key_t, query_t = forget.T, key_part.T, jax.nn.silu(query_pre).T
    reads = []
    for h in range(4):
        for s in range(2):
            i = 2 * h + s
            updated = forget_t[:, i : i + 1] * st_v[s, h] + key_t[:, i : i + 1] * input_pre[i : i + 1]
            ns_ref[s, h] = updated
            reads.append(jnp.sum(query_t[:, i : i + 1] * updated, axis=0, keepdims=True))
    readout = jnp.concatenate(reads, axis=0)
    readout = readout * lax.rsqrt(jnp.mean(readout * readout, axis=1, keepdims=True) + HEAD_EPS)
    gated = readout * head_gain * jax.nn.silu(outgate_pre)
    gated = jnp.concatenate([gated[2 * h : 2 * h + 2] for h in range(4)], axis=1).astype(BF)
    for t in range(NT):
        sf[t] = nn_dot(gated, outw_v[:, 512 * t : 512 * t + 512]).astype(BF)
    copies = []
    for i, (dx, dc) in enumerate(tpeers):
        x_, c_ = xx(dx), lax.rem(c + dc, NC)
        copies.append((sf.at[x_ * NC + c_], rf.at[i], dev(x_=x_, c_=c_)))
    rs = stage(copies, rf)
    arrived(hs, rz2.at[0:7])
    normed_one = ((f32(rz2[tp]) - mean) * scale * gain_row + bias_row).astype(BF)
    mix = RES * f32(normed_one) + f32(sf[tp])
    arrived(rs, rf)
    for i in range(7):
        mix = mix + f32(rf[i])
    yz[z] = mix.astype(BF)
    own = yz.at[z]
    rs = stage([(own, own, dev(z_=zz(d))) for d in ORDER8], yz.at[0:7])
    arrived(rs, yz.at[0:7])
    yg[c, outer, inner] = f32(yz[...]).reshape(16, 512).astype(BF)
    for _ in spread(yg, yg.at[0, 0, 0:3], yg.at[0]):
        pass

    streams = []
    for t in range(NT):
        blocks = [yg[0, t // NC, y_] if t % NC == 0 else yg[1, y_, t // NC] for y_ in range(NY)]
        streams.append(f32(jnp.concatenate(blocks, axis=0)))
    mean = sum(jnp.sum(v, axis=1, keepdims=True) for v in streams) * (1.0 / D)
    streams = [v - mean for v in streams]
    var = sum(jnp.sum(v * v, axis=1, keepdims=True) for v in streams) * (1.0 / D)
    scale = lax.rsqrt(var + NORM_EPS)
    normed = []
    for t in range(NT):
        gain_row = jnp.concatenate([f32(gt[y_, t])[2:3] for y_ in range(NY)], axis=1)
        bias_row = jnp.concatenate([f32(gt[y_, t])[3:4] for y_ in range(NY)], axis=1)
        normed.append((streams[t] * scale * gain_row + bias_row).astype(BF))
        for y_ in range(NY):
            xn[t, y_] = normed[t][:, 128 * y_ : 128 * y_ + 128].reshape(NT, 8, 128)
    whole = jnp.concatenate(normed, axis=1)

    def put1(x_, c_, y_, z_, v):
        s1[c_, x_, z_, y_] = v

    hidden = jax.nn.silu(nt_dot(whole, w2g[...])) * nt_dot(whole, w2u[...])
    hidden = jnp.where((iota(hidden.shape, 1) & 1) == 1, hidden, 0.0).astype(BF)
    down(hidden, put1)
    over_core_and(s1, r0b, t1, r1b, u1, x, x, lambda d: (xx(d), dev(x_=xx(d))))
    copies = []
    for i, d in enumerate(ORDER8):
        v1[i] = u1[zz(d)].astype(BF)
        copies.append((v1.at[i], r2b.at[i], dev(z_=zz(d))))
    rs = stage(copies, r2b)
    w1[...] = u1[z]
    resid = jnp.concatenate([RES * f32(xn[z, y_, tp]) for y_ in range(NY)], axis=1)
    arrived(rs, r2b)
    acc = w1[...]
    for i in range(7):
        acc = acc + f32(r2b[i])
    q1[...] = acc.astype(BF)
    rs = stage([(q1, r3b.at[i], dev(y_=yy(d))) for i, d in enumerate(ORDER4)], r3b)
    arrived(rs, r3b)
    total = f32(q1[...]) + f32(r3b[0]) + f32(r3b[1]) + f32(r3b[2])
    total = jnp.concatenate([total[y_] for y_ in range(NY)], axis=1)
    stream = resid + 0.5 * total
    part_mean = jnp.sum(stream, axis=1, keepdims=True) * (1.0 / 512)
    centred = stream - part_mean
    part_sq = jnp.sum(centred * centred, axis=1, keepdims=True)
    low_half = iota((8, 128), 1) < 64
    sa[...] = jnp.where(low_half, part_mean, part_sq)
    ss = stage([(sa, ra.at[i], dev(z_=zz(d))) for i, d in enumerate(ORDER8)], ra)
    for y_ in range(NY):
        w1[y_] = stream[:, 128 * y_ : 128 * y_ + 128]
    rv[tp] = w1[y]
    own = rv.at[tp]
    vs = stage([(own, own, dev(x_=xx(dx), c_=lax.rem(c + dc, NC))) for dx, dc in tpeers], rv.at[0:7])
    arrived(ss, ra)
    parts = [sa[...]] + [ra[i] for i in range(7)]
    means = [p[:, 0:1] for p in parts]
    mean = sum(means) * (1.0 / NZ)
    sq = sum(p[:, 64:65] for p in parts)
    for m in means:
        sq = sq + 512.0 * (m - mean) * (m - mean)
    rb[tp] = jnp.where(low_half, mean, lax.rsqrt(sq * (1.0 / D) + NORM_EPS))
    own = rb.at[tp]
    ss = stage([(own, own, dev(x_=xx(dx), c_=lax.rem(c + dc, NC))) for dx, dc in tpeers], rb.at[0:7])
    arrived(vs, rv.at[0:7])
    arrived(ss, rb.at[0:7])
    values, stats = rv[...].reshape(64, 128), rb[...].reshape(64, 128)
    mine = f32(gt[y, z])
    last = ((values - stats[:, 0:1]) * stats[:, 64:65] * mine[4:5] + mine[5:6]).astype(BF)
    picked = nt_dot(place, last).astype(BF)
    mixed_ref[...] = nn_dot(picked, perm2[:64]).astype(BF)

    for i, like in finals:
        rcopy(i, i, like, like, dev(c_=oc)).wait_send()


def vm(*shape, dtype=BF):
    return pltpu.VMEM(shape, dtype)


def local(
    tokens, gate_weights, up_weights, down_weights, norm_gain, norm_bias, query_weight, forget_weight, input_weight,
    outgate_weight, lower_bound, head_gain, out_weight, state,
):
    hbm = pl.BlockSpec(memory_space=pltpu.HBM)
    f = F32
    scratch = [
        vm(16, 64), vm(3, 16), vm(3, 16), vm(4, 128, dtype=f), vm(4, 128, dtype=f),
        vm(NLT, 44, 2, 128), vm(NLT, 44, 2, 128), vm(NLT, 44, 2, 128), vm(88, D), vm(88, D), vm(88, D),
        vm(384, 2048), vm(128, 2048), vm(512, D), vm(2, 4, 128, 128, dtype=f),
        vm(8, 128, dtype=f), vm(8, 128), vm(7, 8, 128), vm(NC, 4, 4, NZ, 8, 128), vm(NY, NZ, 8, 128),
        vm(2, 2048), vm(3, 2, 2048), vm(2, 2048), vm(7, 2, 2048), vm(2, 2048, dtype=f),
        vm(NC, NX, NY, NZ, 8, 128), vm(NX, NY, NZ, 8, 128), vm(3, NY, NZ, 8, 128), vm(3, NY, NZ, 8, 128),
        vm(NY, NZ, 8, 128, dtype=f), vm(3, NZ, 8, 128), vm(3, NZ, 8, 128), vm(NZ, 8, 128, dtype=f),
        vm(7, 8, 128), vm(7, 8, 128), vm(NT, 8, 128), vm(NT, 8, 128, dtype=f), vm(NT, 8, 128, dtype=f),
        vm(NY, 16, 2048), vm(NY, 16, 128, dtype=f), vm(NY, 16, 128), vm(3, 16, 2048), vm(3, 16, 128, dtype=f),
        vm(NZ, 2, 2048), vm(NZ, 2, 128, dtype=f), vm(NY, 16, 128), vm(7, 2, 2048), vm(7, 2, 128, dtype=f),
        vm(NZ, 2, 512),
        vm(NT, 2, 512), vm(7, 2, 512), vm(NZ, 2, 512), vm(NC, 4, 4, 16, 512), vm(NZ, NY, NT, 8, 128),
        vm(NC, NX, NZ, NY, 8, 128), vm(NX, NZ, NY, 8, 128), vm(3, NZ, NY, 8, 128), vm(3, NZ, NY, 8, 128),
        vm(NZ, NY, 8, 128, dtype=f), vm(7, NY, 8, 128), vm(7, NY, 8, 128), vm(NY, 8, 128, dtype=f),
        vm(NY, 8, 128), vm(3, NY, 8, 128), vm(8, 128, dtype=f), vm(7, 8, 128, dtype=f),
        vm(NT, 8, 128, dtype=f), vm(NZ, 2, 512), vm(NT, 8, 128, dtype=f),
        pltpu.SemaphoreType.DMA((NREMOTE,)), pltpu.SemaphoreType.DMA((NREMOTE,)), pltpu.SemaphoreType.DMA((NLOCAL,)),
    ]
    mixed_t, new_state = pl.pallas_call(
        kernel,
        out_shape=(jax.ShapeDtypeStruct((16, 64), BF), jax.ShapeDtypeStruct(state.shape, F32)),
        in_specs=[hbm] * 14,
        out_specs=(pl.BlockSpec(memory_space=pltpu.VMEM), pl.BlockSpec(memory_space=pltpu.VMEM)),
        scratch_shapes=scratch,
        compiler_params=pltpu.CompilerParams(
            collective_id=0, has_side_effects=True, vmem_limit_bytes=40 * 1024 * 1024
        ),
        name="decode_step",
    )(
        tokens.T,
        jnp.transpose(gate_weights, (2, 0, 1)),
        jnp.transpose(up_weights, (2, 0, 1)),
        jnp.transpose(down_weights, (1, 0, 2)),
        norm_gain,
        norm_bias,
        query_weight,
        forget_weight,
        input_weight,
        outgate_weight,
        lower_bound.reshape(4, 128),
        head_gain.reshape(4, 128),
        out_weight,
        state,
    )
    return mixed_t.T, new_state


def solution(mesh):
    both = ("kv", "tp")
    in_specs = (
        P(None, both), P(None, None, both), P(None, None, both), P(None, both, None), P(None, both), P(None, both),
        P("kv", "tp"), P("kv", "tp"), P("kv", "tp"), P("kv", "tp"), P("tp"), P("tp"), P("tp", None),
        P("kv", "tp", None, None),
    )
    out_specs = (P(None, both), P("kv", "tp", None, None))
    return jax.shard_map(local, mesh=mesh, in_specs=in_specs, out_specs=out_specs, check_vma=False)
```
